32 devices in a mesh: sp: 8 (over z, x), tp: 4 (over y, core).
Axes of the slice: x: 2, y: 2, z: 4, core: 2. Of those that a mesh axis runs over, the one named last changes fastest.
Arguments:
- residual: bfloat16 [3072, 2048], P(('sp', 'tp')), may hold values from -6 to 6
- queries: bfloat16 [3072, 1024], P('sp', 'tp'), may hold values from -2.5 to 2.5
- keys: bfloat16 [3072, 256], P('sp', 'tp'), may hold values from -2.5 to 2.5
- values: bfloat16 [3072, 256], P('sp', 'tp'), may hold values from -6 to 6
- documents: int32 [3072], P('sp'), may hold values from 0 to 4, never falling along the last dimension, each value on 1 to 1536 neighbouring positions
- sink: float32 [16], P('tp'), may hold values from 3 to 7
- out_weight: bfloat16 [1024, 2048], replicated, may hold values from -0.1875 to 0.1875
- mix_gain: float32 [2048], replicated, may hold values from 0.1 to 1.9
- ffn_gain: float32 [2048], replicated, may hold values from 0.1 to 1.9
- out_gain: float32 [2048], replicated, may hold values from 0.1 to 1.9
- routes: int32 [3072, 4], P(('sp', 'tp')), may hold values from 0 to 7, all different within a row; in each aligned block of 96 rows (0 to 95, 96 to 191, ...) at most 64 rows name the same one
- route_logits: float32 [3072, 4], P(('sp', 'tp')), may hold values from -4 to 4
- gate_weight: bfloat16 [8, 2048, 2048], P('sp', None, 'tp'), may hold values from -1.41421356 to 1.41421356
- up_weight: bfloat16 [8, 2048, 2048], P('sp', None, 'tp'), may hold values from -1.41421356 to 1.41421356
- down_weight: bfloat16 [8, 2048, 2048], P('sp', 'tp'), may hold values from -0.125 to 0.125
Outputs:
- mixed: bfloat16 [3072, 2048], P(('sp', 'tp'))
The draws below stay inside these ranges and needn't reach their ends.
Inputs may be any that keep to these rules, and one draw needn't show every extreme that they name: `routes`: each row names 4 different experts. In each aligned block of rows held by one device, no expert is named by more than 64 rows, a bound that some block reaches. `documents`: document numbers never fall along the positions; each document has 1 to 1536 positions, and one has exactly 1536.
All inputs are finite; a program needn't handle non-finite values.
Results may differ from the reference program's by a relative error of at most 0.017.
Values may be sent and summed in bfloat16 or wider, within the bound.
A program may use at most 128 MiB of HBM per device.

```python
import math
import jax
import jax.numpy as jnp
import numpy as np
from jax import lax

D = 2048
QH = 16
KVH = 4
HD = 64
FF = 2048
TOPK = 4
W = 128
TOK_DEV = 384
TOKENS = 3072
EXPERTS = 8
CAP = 64
DOCS = 5
DOC_MOST = 1536
N_TP = 4


def column_scaled(key):
    base_key, scale_key = jax.random.split(key)
    shape = (EXPERTS, D, FF)
    base = jnp.clip(jax.random.normal(base_key, shape, jnp.float32), -4.0, 4.0)
    column_scale = jnp.exp(jax.random.uniform(scale_key, (EXPERTS, 1, FF), jnp.float32, 0.0, 2.3025851))
    return (base * column_scale * D ** (-0.5)).astype(jnp.bfloat16)


def draw_gate_weight(key, part):
    return column_scaled(jax.random.fold_in(key, 11))


def draw_up_weight(key, part):
    return column_scaled(jax.random.fold_in(key, 23))


def block_scale(own_key, dims, cuts, smallest, high):
    factor_of, own = 1.0, jax.random.fold_in(own_key, 6)
    for dim, parts in cuts:
        heights = jnp.exp(jax.random.uniform(jax.random.fold_in(own, dim), (parts,), jnp.float32, smallest / len(cuts), high / len(cuts)))
        factor_of = factor_of * jnp.repeat(heights, dims[dim] // parts).reshape([-1 if axis == dim else 1 for axis in range(len(dims))])
    return factor_of


def profile(count, total, limit, skew):
    weights = [(1 << 20) // math.isqrt(grade ** skew) + 1 for grade in range(2, count + 1)]
    rest, given = total - limit - (count - 1), [1] * (count - 1)
    while rest > 0:
        free = [i for i in range(count - 1) if given[i] < limit]
        mass, remaining = sum([weights[i] for i in free]), rest
        for i in free:
            addition = min(limit - given[i], max(1, remaining * weights[i] // mass), rest)
            given[i] = given[i] + addition
            rest = rest - addition
    return np.array([limit] + given)


def uneven(own_key, amount, total, limit, skew):
    if amount == 2:
        one = jax.random.randint(own_key, (), max(1, total - limit), min(limit, total - 1) + 1)
        return jnp.stack([one, total - one])
    tallies = jnp.asarray(profile(amount, total, limit, skew), jnp.int32)
    couples = (amount - 1) // 2
    giver, taker = tallies[1:1 + 2 * couples:2], tallies[2:2 + 2 * couples:2]
    margin = jnp.minimum(giver - 1, limit - taker)
    shifted = jax.random.randint(jax.random.fold_in(own_key, 1), (couples,), 0, 1 << 20) % (margin + 1)
    tallies = tallies.at[1:1 + 2 * couples:2].set(giver - shifted).at[2:2 + 2 * couples:2].set(taker + shifted)
    return tallies[jax.random.permutation(jax.random.fold_in(own_key, 2), amount)]


def deal_out(stream_key, own, number, rows, count, top, bound, skew):
    sequence = jax.random.permutation(stream_key, count)
    packed, common = load_shares(count, rows * top, bound, skew, True), load_shares(count, rows * top, bound, skew, False)
    places = jnp.arange(count)

    def named(tallies, turn):
        used = int((tallies > 0).sum())
        fixed = max(1, used // 4)
        moved = fixed + (places - fixed + turn * (used - fixed)) % max(1, count - fixed)
        return jnp.zeros((count,), jnp.int32).at[sequence[jnp.where(places < fixed, places, moved)]].set(jnp.asarray(tallies, jnp.int32))

    tallies = jnp.where(number % 4 == 0, named(packed, number // 4), named(common, number - number // 4 - 1))
    mixed = jax.random.permutation(jax.random.fold_in(own, 3), count)
    giver, taker = mixed[0:count // 2 * 2:2], mixed[1:count // 2 * 2:2]
    slack = jnp.minimum(tallies[giver] - 1, bound - tallies[taker]) // 2
    slack = jnp.where((giver == sequence[0]) | (taker == sequence[0]) | (tallies[taker] == 0), 0, jnp.maximum(slack, 0))
    moved = jax.random.randint(jax.random.fold_in(own, 4), (count // 2,), 0, 1 << 20) % (slack + 1)
    tallies = tallies.at[giver].add(-moved).at[taker].add(moved)
    members = jnp.searchsorted(jnp.cumsum(tallies), jnp.arange(rows * top), side="right").astype(jnp.int32)
    listing = members.reshape(top, rows).T
    listing = listing[jax.random.permutation(jax.random.fold_in(own, 1), rows)]
    turn = jax.random.randint(jax.random.fold_in(own, 2), (rows, 1), 0, top)
    return jnp.take_along_axis(listing, (jnp.arange(top)[None, :] + turn) % top, axis=1)


def load_shares(number_of, total, limit, skew, full):
    weights = [(1 << 20) // math.isqrt(rank ** skew) + 1 for rank in range(1, number_of + 1)]
    largest = limit if full else min(limit, max(-(-total // number_of), total * weights[0] // sum(weights)))
    least = 1 if total - largest >= number_of - 1 else 0
    given, rest = [largest] + [least] * (number_of - 1), total - largest - least * (number_of - 1)
    while rest > 0:
        candidates = [i for i in range(1, number_of) if given[i] < largest] or [i for i in range(1, number_of) if given[i] < limit]
        mass, budget = sum([weights[i] for i in candidates]), rest
        for i in candidates:
            more = min(limit - given[i], max(1, budget * weights[i] // mass), rest)
            given[i] = given[i] + more
            rest = rest - more
    return np.array(given)


def noise(key, shape, width, most, shards=(), kind=jnp.bfloat16):
    array = jax.random.normal(key, shape, jnp.float32) * width
    if len(shards) > 0:
        array = block_scale(key, shape, shards, -0.22, 0.18) * array
    return jnp.clip(array, min=-most, max=most).astype(kind)


def setup_inputs(seed: int = 0) -> dict:
    splits = jax.random.split(jax.random.key(seed), 16)
    residual = noise(splits[0], (TOKENS, D), 1.0, 6.0, ((0, 32),))
    queries = noise(splits[1], (TOKENS, QH * HD), 1.0, 2.5, ((0, 8), (1, 4)))
    keys = noise(splits[2], (TOKENS, KVH * HD), 1.0, 2.5, ((0, 8), (1, 4)))
    values = noise(splits[3], (TOKENS, KVH * HD), 1.0, 6.0, ((0, 8), (1, 4)))
    documents = jnp.searchsorted(jnp.cumsum(uneven(splits[4], DOCS, TOKENS, DOC_MOST, 1)), jnp.arange(TOKENS), side="right").astype(jnp.int32)
    sink = jnp.clip(3.0 + 4.0 * jax.random.uniform(splits[5], (QH,), jnp.float32) ** block_scale(splits[5], (QH,), ((0, 4),), -0.2, 0.2), 3.0, 7.0)
    out_weight = noise(splits[6], (QH * HD, D), (QH * HD) ** -0.5, 0.1875)
    mix_gain = jnp.clip(1.0 + 0.18 * jax.random.normal(splits[7], (D,), jnp.float32), 0.1, 1.9)
    ffn_gain = jnp.clip(1.0 + 0.18 * jax.random.normal(splits[8], (D,), jnp.float32), 0.1, 1.9)
    out_gain = jnp.clip(1.0 + 0.18 * jax.random.normal(splits[9], (D,), jnp.float32), 0.1, 1.9)
    routes_keys = jax.random.split(jax.random.fold_in(splits[10], 1), TOKENS // (TOK_DEV // N_TP))
    routes_turns = jax.random.permutation(jax.random.fold_in(splits[10], 3), TOKENS // (TOK_DEV // N_TP))
    routes = jax.vmap(lambda own, number: deal_out(jax.random.fold_in(splits[10], 2), own, number, TOK_DEV // N_TP, EXPERTS, TOPK, CAP, 2))(routes_keys, routes_turns).reshape((TOKENS, TOPK))
    route_logits = noise(splits[11], (TOKENS, TOPK), 1.0, 4.0, ((0, 32),), jnp.float32)
    gate_weight = draw_gate_weight(jax.random.fold_in(splits[15], 71), 0)
    up_weight = draw_up_weight(jax.random.fold_in(splits[15], 71), 0)
    down_weight = noise(splits[14], (EXPERTS, FF, D), FF ** -0.5, 0.125, ((0, 8), (1, 4)))
    return {"residual": residual, "queries": queries, "keys": keys, "values": values, "documents": documents, "sink": sink, "out_weight": out_weight, "mix_gain": mix_gain, "ffn_gain": ffn_gain, "out_gain": out_gain, "routes": routes, "route_logits": route_logits, "gate_weight": gate_weight, "up_weight": up_weight, "down_weight": down_weight}


def turn_heads(block, positions, head_count):
    total = block.shape[0]
    heads = block.astype(jnp.float32).reshape(total, head_count, HD)
    half_size = HD // 2
    inverse = 10000.0 ** (-jnp.arange(half_size, dtype=jnp.float32) / half_size)
    angles = positions.astype(jnp.float32)[:, None] * inverse[None, :]
    cosine = jnp.cos(angles)[:, None, :]
    sine = jnp.sin(angles)[:, None, :]
    first_half = heads[..., :half_size]
    second_half = heads[..., half_size:]
    turned = jnp.concatenate([first_half * cosine - second_half * sine, second_half * cosine + first_half * sine], axis=-1)
    return turned.reshape(total, head_count * HD).astype(jnp.bfloat16)

def rms_scale(vector):
    return vector * lax.rsqrt(lax.optimization_barrier(jnp.mean(vector * vector, axis=-1, keepdims=True)) + 1e-06)

def windows(padded_rows, blocks):
    tiled = padded_rows.reshape((blocks + 2, W) + padded_rows.shape[1:])
    return jnp.concatenate([tiled[:-2], tiled[1:-1], tiled[2:]], axis=1)

def reference(residual, queries, keys, values, documents, sink, out_weight, mix_gain, ffn_gain, out_gain, routes, route_logits, gate_weight, up_weight, down_weight):
    total = TOKENS
    group_size = QH // KVH
    positions = jnp.arange(total, dtype=jnp.int32)
    q_turned = turn_heads(queries, positions, QH)
    k_turned = turn_heads(keys, positions, KVH)
    blocks = total // W
    query_blocks = q_turned.reshape(blocks, W, KVH, group_size, HD)
    key_pad = jnp.pad(k_turned.reshape(total, KVH, HD), ((W, W), (0, 0), (0, 0)))
    value_pad = jnp.pad(values.reshape(total, KVH, HD), ((W, W), (0, 0), (0, 0)))
    doc_pad = jnp.pad(documents, (W, W), constant_values=-1)
    key_win = windows(key_pad, blocks)
    value_win = windows(value_pad, blocks)
    doc_win = windows(doc_pad, blocks)
    doc_query = documents.reshape(blocks, W)
    block_ids = jnp.arange(blocks, dtype=jnp.int32)[:, None, None]
    query_pos = block_ids * W + jnp.arange(W, dtype=jnp.int32)[None, :, None]
    key_pos = (block_ids - 1) * W + jnp.arange(3 * W, dtype=jnp.int32)[None, None, :]
    keep_mask = (jnp.abs(query_pos - key_pos) <= W) & (key_pos >= 0) & (key_pos < total)
    keep_mask = keep_mask & (doc_query[:, :, None] == doc_win[:, None, :])
    sink_terms = jnp.exp(sink).reshape(KVH, group_size, 1, 1)

    def one_block(operands):
        query_one, key_one, value_one, mask_one = operands
        scores = jnp.einsum('qhgd,khd->hgqk', query_one.astype(jnp.float32), key_one.astype(jnp.float32)) * HD ** (-0.5)
        exponent = jnp.where(mask_one[None, None], jnp.exp(scores), 0.0)
        denominator = lax.optimization_barrier(jnp.sum(exponent, axis=-1, keepdims=True)) + sink_terms
        probs = (exponent / denominator).astype(jnp.bfloat16)
        attended_one = jnp.einsum('hgqk,khd->qhgd', probs.astype(jnp.float32), value_one.astype(jnp.float32))
        return attended_one.astype(jnp.bfloat16).reshape(W, QH * HD)
    attended = lax.map(one_block, (query_blocks, key_win, value_win, keep_mask)).reshape(total, QH * HD)
    projected = jnp.dot(attended, out_weight, preferred_element_type=jnp.float32)
    after_mix = residual.astype(jnp.float32) + rms_scale(projected) * mix_gain
    normed = (rms_scale(after_mix) * ffn_gain).astype(jnp.bfloat16)
    row_block = 128
    assigned = total * TOPK
    flat_routes = routes.reshape(assigned).astype(jnp.int32)
    order = jnp.argsort(flat_routes, stable=True).astype(jnp.int32)
    sorted_experts = flat_routes[order]
    sorted_tokens = (order // TOPK).astype(jnp.int32)
    counts = lax.optimization_barrier(jnp.sum((flat_routes[:, None] == jnp.arange(EXPERTS, dtype=jnp.int32)[None, :]).astype(jnp.int32), axis=0))
    padded_counts = (counts + row_block - 1) // row_block * row_block
    starts = jnp.cumsum(counts) - counts
    padded_ends = jnp.cumsum(padded_counts)
    padded_starts = padded_ends - padded_counts
    slot_rows = (padded_starts[sorted_experts] + jnp.arange(assigned, dtype=jnp.int32) - starts[sorted_experts]).astype(jnp.int32)
    block_count = -(-(assigned + EXPERTS * (row_block - 1)) // row_block)
    padded_total = block_count * row_block
    row_token = jnp.full((padded_total,), total, dtype=jnp.int32).at[slot_rows].set(sorted_tokens)
    with_zero = jnp.concatenate([normed, jnp.zeros((1, D), jnp.bfloat16)], axis=0)
    expert_rows = with_zero[row_token].reshape(block_count, row_block, D)
    block_expert = jnp.minimum(jnp.searchsorted(padded_ends, jnp.arange(block_count, dtype=jnp.int32) * row_block, side='right'), EXPERTS - 1).astype(jnp.int32)
    quarter = FF // N_TP

    def expert_block(operands):
        rows_in, expert_id = operands
        gate_pre = jnp.dot(rows_in, gate_weight[expert_id], preferred_element_type=jnp.float32)
        up_pre = jnp.dot(rows_in, up_weight[expert_id], preferred_element_type=jnp.float32)
        gated = jnp.minimum(gate_pre, 7.0)
        upper = jnp.clip(up_pre, -7.0, 7.0)
        hidden = ((upper + 1.0) * gated * jax.nn.sigmoid(1.702 * gated)).astype(jnp.bfloat16)
        down_one = down_weight[expert_id]
        summed = jnp.zeros((rows_in.shape[0], D), jnp.float32)
        for source in range(N_TP):
            partial_out = jnp.dot(hidden[:, source * quarter:(source + 1) * quarter], down_one[source * quarter:(source + 1) * quarter], preferred_element_type=jnp.float32)
            summed = summed + lax.optimization_barrier(partial_out.astype(jnp.bfloat16)).astype(jnp.float32)
        return summed.astype(jnp.bfloat16)
    expert_out = lax.map(expert_block, (expert_rows, block_expert)).reshape(padded_total, D)
    row_of = jnp.zeros((assigned,), jnp.int32).at[order].set(slot_rows).reshape(total, TOPK)
    exp_logits = jnp.exp(route_logits)
    route_weights = exp_logits / lax.optimization_barrier(jnp.sum(exp_logits, axis=-1, keepdims=True))
    expert_mix = jnp.zeros((total, D), jnp.float32)
    for choice_index in range(TOPK):
        expert_mix = expert_mix + route_weights[:, choice_index:choice_index + 1] * expert_out[row_of[:, choice_index]].astype(jnp.float32)
    return (after_mix + rms_scale(expert_mix) * out_gain).astype(jnp.bfloat16)
```

```python
import functools

import jax
import jax.numpy as jnp
from jax import lax
from jax.experimental import pallas as pl
from jax.experimental.pallas import tpu as pltpu
from jax.sharding import PartitionSpec as P

HD = 64
TOPK = 4
W = 128


def extended(block, sides, width):
    for axis, dim in sides:
        count = lax.axis_size(axis)
        forward = [(i, i + 1) for i in range(count - 1)]
        backward = [(target, source) for source, target in forward]
        low = lax.ppermute(
            lax.slice_in_dim(block, block.shape[dim] - width, None, axis=dim), axis, forward
        )
        high = lax.ppermute(lax.slice_in_dim(block, 0, width, axis=dim), axis, backward)
        block = jnp.concatenate([low, block, high], axis=dim)
    return block


def turn_heads(block, positions, head_count):
    total = block.shape[0]
    heads = block.astype(jnp.float32).reshape(total, head_count, HD)
    half_size = HD // 2
    inverse = 10000.0 ** (-jnp.arange(half_size, dtype=jnp.float32) / half_size)
    angles = positions.astype(jnp.float32)[:, None] * inverse[None, :]
    cosine = jnp.cos(angles)[:, None, :]
    sine = jnp.sin(angles)[:, None, :]
    first_half = heads[..., :half_size]
    second_half = heads[..., half_size:]
    turned = jnp.concatenate(
        [first_half * cosine - second_half * sine, second_half * cosine + first_half * sine],
        axis=-1,
    )
    return turned.reshape(total, head_count * HD).astype(jnp.bfloat16)


def rms_scale(vector):
    return vector * lax.rsqrt(jnp.mean(vector * vector, axis=-1, keepdims=True) + 1e-06)


def windows(padded_rows, blocks):
    tiled = padded_rows.reshape((blocks + 2, W) + padded_rows.shape[1:])
    return jnp.concatenate([tiled[:-2], tiled[1:-1], tiled[2:]], axis=1)


def flipped(index, bits, size):
    result, unit = 0, 1
    while unit < size:
        result = result + ((index // unit + bits // unit) % 2) * unit
        unit *= 2
    return result


def expert_kernel(
    sp_count, tp_count, capacity,
    outgoing, gate_hbm, up_hbm, down_hbm,
    returned,
    gate, up, down, rows, part, core_in, y_out, y_in, done_out,
    weight_sem, local_sem, send_sem, recv_sem,
):
    me = lax.axis_index("sp")
    tp = lax.axis_index("tp")
    mate = flipped(tp, 1, tp_count)
    across = flipped(tp, 2, tp_count)
    SP, ACROSS, NEAR, NEAR2, CORE, BACK, HOME = range(7)

    def remote(kind, step, source, target, device):
        return pltpu.make_async_remote_copy(
            src_ref=source,
            dst_ref=target,
            send_sem=send_sem.at[kind, step],
            recv_sem=recv_sem.at[kind, step],
            device_id=device,
            device_id_type=pl.DeviceIdType.MESH,
        )

    def out_copy(step):
        peer = flipped(me, step, sp_count)
        return remote(SP, step, outgoing.at[peer], rows.at[step, 0], {"sp": peer})

    def across_copy(step):
        return remote(ACROSS, step, rows.at[step, 0], rows.at[step, 1], {"tp": across})

    def near_copy(step):
        return remote(NEAR, step, rows.at[step, 0], rows.at[step, 2], {"tp": mate})

    def near2_copy(step):
        return remote(NEAR2, step, rows.at[step, 1], rows.at[step, 3], {"tp": mate})

    def core_copy(step):
        return remote(CORE, step, part.at[step, pl.ds(2, 2)], core_in.at[step], {"tp": mate})

    def back_copy(step):
        return remote(BACK, step, y_out.at[step], y_in.at[step], {"tp": across})

    def home_copy(step):
        peer = flipped(me, step, sp_count)
        return remote(HOME, step, done_out.at[step], returned.at[me], {"sp": peer})

    weights = [
        pltpu.make_async_copy(source, target, weight_sem.at[n])
        for n, (source, target) in enumerate(((gate_hbm, gate), (up_hbm, up), (down_hbm, down)))
    ]
    own_in = pltpu.make_async_copy(outgoing.at[me], rows.at[0, 0], local_sem.at[0])
    own_out = pltpu.make_async_copy(done_out.at[0], returned.at[me], local_sem.at[1])

    barrier = pltpu.get_barrier_semaphore()
    own_in.start()

    def greet(step, carry):
        pl.semaphore_signal(
            barrier, inc=1, device_id={"sp": flipped(me, step, sp_count)},
            device_id_type=pl.DeviceIdType.MESH,
        )
        return carry

    lax.fori_loop(1, sp_count, greet, 0)
    for near in (mate, across):
        pl.semaphore_signal(
            barrier, inc=1, device_id={"tp": near}, device_id_type=pl.DeviceIdType.MESH
        )
    pl.semaphore_wait(barrier, sp_count + 1)

    def send_out(step, carry):
        out_copy(step).start()
        return carry

    lax.fori_loop(1, sp_count, send_out, 0)
    for copy in weights:
        copy.start()
    own_in.wait()

    local_experts, width, units = gate.shape
    slots = rows.shape[2]
    chunk = tp_count * slots

    def forward(step):
        @pl.when(step > 0)
        def _():
            out_copy(step).wait_recv()

        across_copy(step).start()
        near_copy(step).start()

    def forward_again(step):
        across_copy(step).wait_recv()
        near2_copy(step).start()

    def compute(step):
        @pl.when(step == 0)
        def _():
            for copy in weights:
                copy.wait()

        near_copy(step).wait_recv()
        near2_copy(step).wait_recv()
        block = rows[step].reshape(chunk, width)
        hiddens = []
        for expert in range(local_experts):
            gate_pre = jnp.dot(block, gate[expert], preferred_element_type=jnp.float32)
            up_pre = jnp.dot(block, up[expert], preferred_element_type=jnp.float32)
            gated = jnp.minimum(gate_pre, 7.0)
            upper = jnp.clip(up_pre, -7.0, 7.0)
            hidden = (upper + 1.0) * gated * jax.nn.sigmoid(1.702 * gated)
            if local_experts > 1:
                row = lax.broadcasted_iota(jnp.int32, (chunk, units), 0)
                hidden = jnp.where((row // capacity) % local_experts == expert, hidden, 0.0)
            hiddens.append(hidden.astype(jnp.bfloat16))
        tile = width // 4
        for start in range(0, width, tile):
            total = jnp.dot(
                hiddens[0], down[0, :, start : start + tile], preferred_element_type=jnp.float32
            )
            for expert in range(1, local_experts):
                total = total + jnp.dot(
                    hiddens[expert], down[expert, :, start : start + tile],
                    preferred_element_type=jnp.float32,
                )
            part[step, :, :, start : start + tile] = total.astype(jnp.bfloat16).reshape(
                tp_count, slots, tile
            )
        core_copy(step).start()

    def add_core(step):
        core_copy(step).wait_recv()
        y_out[step] = (
            part[step, 1].astype(jnp.float32) + core_in[step, 1].astype(jnp.float32)
        ).astype(jnp.bfloat16)
        back_copy(step).start()

    def add_across(step):
        back_copy(step).wait_recv()
        done_out[step] = (
            part[step, 0].astype(jnp.float32)
            + core_in[step, 0].astype(jnp.float32)
            + y_in[step].astype(jnp.float32)
        ).astype(jnp.bfloat16)

        @pl.when(step == 0)
        def _():
            own_out.start()

        @pl.when(step > 0)
        def _():
            home_copy(step).start()

    stages = ((forward_again, 1), (compute, 2), (add_core, 3), (add_across, 4), (forward, 0))

    def turn(number, carry):
        for stage, lag in stages:
            step = number - lag

            @pl.when((step >= 0) & (step < sp_count))
            def _():
                stage(step)

        return carry

    lax.fori_loop(0, sp_count + 4, turn, 0)

    def finish(step, carry):
        @pl.when(step > 0)
        def _():
            out_copy(step).wait_send()
            home_copy(step).wait_send()
            home_copy(step).wait_recv()

        for make in (across_copy, near_copy, near2_copy, core_copy, back_copy):
            make(step).wait_send()
        return carry

    lax.fori_loop(0, sp_count, finish, 0)
    own_out.wait()


def run_experts(outgoing, gate_weight, up_weight, down_weight, capacity):
    sp_count, slots, width = outgoing.shape
    tp_count = lax.axis_size("tp")
    assert tp_count == 4
    local_experts, _, units = gate_weight.shape
    rows = sp_count * tp_count * slots
    half = jnp.bfloat16
    anywhere = pl.BlockSpec(memory_space=pl.ANY)
    return pl.pallas_call(
        functools.partial(expert_kernel, sp_count, tp_count, capacity),
        out_shape=jax.ShapeDtypeStruct(outgoing.shape, half),
        in_specs=[anywhere] * 4,
        out_specs=anywhere,
        scratch_shapes=[
            pltpu.VMEM(gate_weight.shape, half),
            pltpu.VMEM(up_weight.shape, half),
            pltpu.VMEM(down_weight.shape, half),
            pltpu.VMEM((sp_count, tp_count, slots, width), half),
            pltpu.VMEM((sp_count, tp_count, slots, width), half),
            pltpu.VMEM((sp_count, 2, slots, width), half),
            pltpu.VMEM((sp_count, slots, width), half),
            pltpu.VMEM((sp_count, slots, width), half),
            pltpu.VMEM((sp_count, slots, width), half),
            pltpu.SemaphoreType.DMA((3,)),
            pltpu.SemaphoreType.DMA((2,)),
            pltpu.SemaphoreType.DMA((7, sp_count)),
            pltpu.SemaphoreType.DMA((7, sp_count)),
        ],
        compiler_params=pltpu.CompilerParams(
            collective_id=0, has_side_effects=True, vmem_limit_bytes=60 * 1024 * 1024
        ),
        cost_estimate=pl.CostEstimate(
            flops=6 * rows * local_experts * width * units,
            bytes_accessed=6 * local_experts * width * units,
            transcendentals=rows * units,
        ),
        name="experts",
    )(outgoing, gate_weight, up_weight, down_weight)


def body(
    residual,
    queries,
    keys,
    values,
    documents,
    sink,
    out_weight,
    mix_gain,
    ffn_gain,
    out_gain,
    routes,
    route_logits,
    gate_weight,
    up_weight,
    down_weight,
):
    tok_rows = queries.shape[0]
    head_count = queries.shape[1] // HD
    kv_count = keys.shape[1] // HD
    group_size = head_count // kv_count
    sp_count = lax.axis_size("sp")
    tp_count = lax.axis_size("tp")
    offset = lax.axis_index("sp") * tok_rows
    positions = offset + jnp.arange(tok_rows, dtype=jnp.int32)
    q_turned = turn_heads(queries, positions, head_count)
    k_turned = turn_heads(keys, positions, kv_count)
    paired = jnp.concatenate([k_turned, values], axis=1)
    wide_pairs, wide_docs = (
        extended(paired, (("sp", 0),), W),
        extended(documents, (("sp", 0),), W),
    )
    blocks = tok_rows // W
    query_blocks = q_turned.reshape(blocks, W, kv_count, group_size, HD)
    pair_win = windows(wide_pairs, blocks)
    key_win = pair_win[..., : kv_count * HD].reshape(blocks, 3 * W, kv_count, HD)
    value_win = pair_win[..., kv_count * HD :].reshape(blocks, 3 * W, kv_count, HD)
    doc_win = windows(wide_docs, blocks)
    doc_query = documents.reshape(blocks, W)
    block_ids = jnp.arange(blocks, dtype=jnp.int32)[:, None, None]
    query_pos = offset + block_ids * W + jnp.arange(W, dtype=jnp.int32)[None, :, None]
    key_pos = offset + (block_ids - 1) * W + jnp.arange(3 * W, dtype=jnp.int32)[None, None, :]
    keep_mask = (
        (jnp.abs(query_pos - key_pos) <= W) & (key_pos >= 0) & (key_pos < tok_rows * sp_count)
    )
    keep_mask = keep_mask & (doc_query[:, :, None] == doc_win[:, None, :])
    scores = jnp.einsum(
        "nqhgd,nkhd->nhgqk", query_blocks, key_win, preferred_element_type=jnp.float32
    ) * HD ** (-0.5)
    exponent = jnp.where(keep_mask[:, None, None], jnp.exp(scores), 0.0)
    denominator = jnp.sum(exponent, axis=-1, keepdims=True) + jnp.exp(sink).reshape(
        1, kv_count, group_size, 1, 1
    )
    probs = (exponent / denominator).astype(jnp.bfloat16)
    attended = jnp.einsum("nhgqk,nkhd->nqhgd", probs, value_win, preferred_element_type=jnp.float32)
    attended = attended.astype(jnp.bfloat16).reshape(tok_rows, head_count * HD)
    own_rows = tok_rows // tp_count
    all_heads = lax.all_to_all(attended, "tp", split_axis=0, concat_axis=1, tiled=True)
    projected = jnp.dot(all_heads, out_weight, preferred_element_type=jnp.float32)
    after_mix = residual.astype(jnp.float32) + rms_scale(projected) * mix_gain
    normed = (rms_scale(after_mix) * ffn_gain).astype(jnp.bfloat16)
    local_experts = gate_weight.shape[0]
    expert_count = local_experts * sp_count
    capacity = max(2, own_rows * TOPK * 4 // (3 * expert_count))
    exp_logits = jnp.exp(route_logits)
    route_weights = exp_logits / jnp.sum(exp_logits, axis=-1, keepdims=True)
    named = routes[:, :, None] == jnp.arange(expert_count, dtype=jnp.int32)
    hits = jnp.any(named, axis=1)
    expert_weights = jnp.sum(jnp.where(named, route_weights[:, :, None], 0.0), axis=1)
    row_ids = jnp.arange(own_rows, dtype=jnp.int32)
    lower = (row_ids[:, None] >= row_ids[None, :]).astype(jnp.bfloat16)
    places = jnp.dot(lower, hits.astype(jnp.bfloat16), preferred_element_type=jnp.float32)
    places = jnp.where(hits, places.astype(jnp.int32) - 1, -1)
    slot_ids = jnp.arange(capacity, dtype=jnp.int32)
    total_slots = expert_count * capacity
    chosen = places[:, :, None] == slot_ids
    pick = (places.T[:, None, :] == slot_ids[None, :, None]).reshape(total_slots, own_rows)
    outgoing = jnp.dot(
        pick.astype(jnp.bfloat16), normed, preferred_element_type=jnp.float32
    ).astype(jnp.bfloat16)
    model_width = normed.shape[1]
    outgoing = outgoing.reshape(sp_count, local_experts * capacity, model_width)
    returned = run_experts(outgoing, gate_weight, up_weight, down_weight, capacity)
    returned = returned.reshape(total_slots, model_width)
    high = expert_weights.astype(jnp.bfloat16).astype(jnp.float32)
    low = expert_weights - high

    def spread(weights):
        wide = jnp.where(chosen, weights[:, :, None], 0.0)
        return wide.reshape(own_rows, total_slots).astype(jnp.bfloat16)

    expert_mix = jnp.dot(spread(high), returned, preferred_element_type=jnp.float32)
    expert_mix = expert_mix + jnp.dot(spread(low), returned, preferred_element_type=jnp.float32)
    return (after_mix + rms_scale(expert_mix) * out_gain).astype(jnp.bfloat16)


def solution(mesh):
    in_specs = (
        P(("sp", "tp"), None),
        P("sp", "tp"),
        P("sp", "tp"),
        P("sp", "tp"),
        P("sp"),
        P("tp"),
        P(),
        P(),
        P(),
        P(),
        P(("sp", "tp"), None),
        P(("sp", "tp"), None),
        P("sp", None, "tp"),
        P("sp", None, "tp"),
        P("sp", "tp", None),
    )
    out_specs = P(("sp", "tp"), None)
    return jax.shard_map(body, mesh=mesh, in_specs=in_specs, out_specs=out_specs, check_vma=False)
```

```python
import functools

import jax
import jax.numpy as jnp
from jax import lax
from jax.experimental import pallas as pl
from jax.experimental.pallas import tpu as pltpu
from jax.sharding import PartitionSpec as P

HD = 64
TOPK = 4
W = 128


def rms_scale(vector):
    return vector * lax.rsqrt(jnp.mean(vector * vector, axis=-1, keepdims=True) + 1e-06)


def attention_kernel(
    sp_count, tp_count,
    queries, keys, values, documents, doc_column, cosine, sine, sink_terms,
    heads_out,
    wide_keys, wide_values, wide_docs, turned_keys, attended,
    local_sem, send_sem, recv_sem, out_send, out_recv,
):
    me = lax.axis_index("sp")
    tp = lax.axis_index("tp")
    right = (me + 1) % sp_count
    left = (me + sp_count - 1) % sp_count
    tok_rows, width = queries.shape
    blocks = tok_rows // W
    kv_count = keys.shape[1] // HD
    group_size = width // HD // kv_count
    own_rows = tok_rows // tp_count
    total = tok_rows * sp_count
    mesh_id = pl.DeviceIdType.MESH

    inside = pl.ds(W, tok_rows)
    locals_in = [
        pltpu.make_async_copy(source, target, local_sem.at[n])
        for n, (source, target) in enumerate(
            (
                (keys, wide_keys.at[inside]),
                (values, wide_values.at[inside]),
                (documents, wide_docs.at[pl.ds(1, blocks)]),
            )
        )
    ]
    for copy in locals_in:
        copy.start()

    barrier = pltpu.get_barrier_semaphore()
    for neighbour in (left, right):
        pl.semaphore_signal(barrier, inc=1, device_id={"sp": neighbour}, device_id_type=mesh_id)
    for hop in range(1, tp_count):
        pl.semaphore_signal(
            barrier, inc=1, device_id={"tp": (tp + hop) % tp_count}, device_id_type=mesh_id
        )
    pl.semaphore_wait(barrier, 2 + tp_count - 1)

    low, high = pl.ds(0, W), pl.ds(tok_rows + W, W)
    last = pl.ds(tok_rows - W, W)
    pairs = (
        (keys.at[last], wide_keys.at[low], right),
        (values.at[last], wide_values.at[low], right),
        (documents.at[blocks - 1], wide_docs.at[0], right),
        (keys.at[low], wide_keys.at[high], left),
        (values.at[low], wide_values.at[high], left),
        (documents.at[0], wide_docs.at[blocks + 1], left),
    )
    halos = [
        pltpu.make_async_remote_copy(
            src_ref=source, dst_ref=target, send_sem=send_sem.at[n], recv_sem=recv_sem.at[n],
            device_id={"sp": device}, device_id_type=mesh_id,
        )
        for n, (source, target, device) in enumerate(pairs)
    ]
    for copy in halos:
        copy.start()

    def turn(block, rows):
        size = block.shape[1]
        wide = block.astype(jnp.float32)
        lane = lax.broadcasted_iota(jnp.int32, block.shape, 1)
        swapped = jnp.where(
            lane % HD < HD // 2, jnp.roll(wide, -(HD // 2), 1), jnp.roll(wide, HD // 2, 1)
        )
        copies = size // HD
        cos = jnp.concatenate([cosine[rows, :]] * copies, axis=1)
        sin = jnp.concatenate([sine[rows, :]] * copies, axis=1)
        return (wide * cos + swapped * sin).astype(jnp.bfloat16)

    turned_queries = [
        turn(queries[n * W : (n + 1) * W, :], slice((n + 1) * W, (n + 2) * W))
        for n in range(blocks)
    ]
    for copy in locals_in:
        copy.wait()
    for copy in halos:
        copy.wait()
    for n in range(blocks + 2):
        rows = slice(n * W, (n + 1) * W)
        turned_keys[rows, :] = turn(wide_keys[rows, :], rows)

    scale = HD ** (-0.5)
    for n in range(blocks):
        start = me * tok_rows + n * W
        query_pos = lax.broadcasted_iota(jnp.int32, (W, 3 * W), 0) + W
        key_pos = lax.broadcasted_iota(jnp.int32, (W, 3 * W), 1)
        place = key_pos + (start - W)
        doc_keys = jnp.concatenate([wide_docs[n + m] for m in range(3)], axis=1)
        keep = (jnp.abs(query_pos - key_pos) <= W) & (place >= 0) & (place < total)
        keep = keep & (doc_column[n * W : (n + 1) * W, :] == doc_keys)
        for head in range(kv_count * group_size):
            kv = slice(head // group_size * HD, (head // group_size + 1) * HD)
            columns = slice(head * HD, (head + 1) * HD)
            window = slice(n * W, (n + 3) * W)
            scores = lax.dot_general(
                turned_queries[n][:, columns], turned_keys[window, kv],
                (((1,), (1,)), ((), ())), preferred_element_type=jnp.float32,
            ) * scale
            exponent = jnp.where(keep, jnp.exp(scores), 0.0)
            denominator = jnp.sum(exponent, axis=-1, keepdims=True) + sink_terms[head]
            probs = (exponent / denominator).astype(jnp.bfloat16)
            found = jnp.dot(probs, wide_values[window, kv], preferred_element_type=jnp.float32)
            attended[n * W : (n + 1) * W, columns] = found.astype(jnp.bfloat16)

    def share(index):
        return attended.at[pl.ds(pl.multiple_of(index * own_rows, own_rows), own_rows)]

    mine = heads_out.at[:, pl.ds(pl.multiple_of(tp * width, width), width)]
    sends = []
    for hop in range(1, tp_count):
        peer = (tp + hop) % tp_count
        sends.append(
            pltpu.make_async_remote_copy(
                src_ref=share(peer), dst_ref=mine, send_sem=out_send.at[hop],
                recv_sem=out_recv.at[hop], device_id={"tp": peer}, device_id_type=mesh_id,
            )
        )
    for copy in sends:
        copy.start()
    own = pltpu.make_async_copy(share(tp), mine, local_sem.at[3])
    own.start()
    own.wait()
    for copy in sends:
        copy.wait()


def run_attention(queries, keys, values, documents, sink):
    sp_count = lax.axis_size("sp")
    tp_count = lax.axis_size("tp")
    tok_rows, width = queries.shape
    blocks = tok_rows // W
    half_size = HD // 2
    first = lax.axis_index("sp") * tok_rows - W
    positions = first + jnp.arange(tok_rows + 2 * W, dtype=jnp.int32)
    inverse = 10000.0 ** (-jnp.arange(half_size, dtype=jnp.float32) / half_size)
    angles = positions.astype(jnp.float32)[:, None] * inverse[None, :]
    cosine, sine = jnp.cos(angles), jnp.sin(angles)
    cosine = jnp.concatenate([cosine, cosine], axis=1)
    sine = jnp.concatenate([-sine, sine], axis=1)
    vmem = pl.BlockSpec(memory_space=pltpu.VMEM)
    anywhere = pl.BlockSpec(memory_space=pl.ANY)
    half = jnp.bfloat16
    wide = tok_rows + 2 * W
    return pl.pallas_call(
        functools.partial(attention_kernel, sp_count, tp_count),
        out_shape=jax.ShapeDtypeStruct((tok_rows // tp_count, width * tp_count), half),
        in_specs=[vmem, anywhere, anywhere, anywhere, vmem, vmem, vmem,
                  pl.BlockSpec(memory_space=pltpu.SMEM)],
        out_specs=vmem,
        scratch_shapes=[
            pltpu.VMEM((wide, keys.shape[1]), half),
            pltpu.VMEM((wide, keys.shape[1]), half),
            pltpu.VMEM((blocks + 2, 1, W), jnp.int32),
            pltpu.VMEM((wide, keys.shape[1]), half),
            pltpu.VMEM((tok_rows, width), half),
            pltpu.SemaphoreType.DMA((4,)),
            pltpu.SemaphoreType.DMA((6,)),
            pltpu.SemaphoreType.DMA((6,)),
            pltpu.SemaphoreType.DMA((tp_count,)),
            pltpu.SemaphoreType.DMA((tp_count,)),
        ],
        compiler_params=pltpu.CompilerParams(collective_id=1, has_side_effects=True),
        cost_estimate=pl.CostEstimate(
            flops=4 * tok_rows * 3 * W * width,
            bytes_accessed=4 * tok_rows * width,
            transcendentals=tok_rows * 3 * W * width // HD,
        ),
        name="attention",
    )(
        queries, keys, values, documents.reshape(blocks, 1, W), documents[:, None],
        cosine, sine, jnp.exp(sink),
    )


def flipped(index, bits, size):
    result, unit = 0, 1
    while unit < size:
        result = result + ((index // unit + bits // unit) % 2) * unit
        unit *= 2
    return result


def expert_kernel(
    sp_count, tp_count, capacity,
    outgoing, gate_hbm, up_hbm, down_hbm,
    returned,
    gate, up, down, rows, part, core_in, y_out, y_in, done_out,
    weight_sem, local_sem, send_sem, recv_sem,
):
    me = lax.axis_index("sp")
    tp = lax.axis_index("tp")
    mate = flipped(tp, 1, tp_count)
    across = flipped(tp, 2, tp_count)
    SP, ACROSS, NEAR, NEAR2, CORE, BACK, HOME = range(7)

    def bits_of(step):
        return step // 2 + (step % 2) * (sp_count // 2)

    def remote(kind, step, source, target, device):
        return pltpu.make_async_remote_copy(
            src_ref=source,
            dst_ref=target,
            send_sem=send_sem.at[kind, step],
            recv_sem=recv_sem.at[kind, step],
            device_id=device,
            device_id_type=pl.DeviceIdType.MESH,
        )

    def out_copy(step):
        peer = flipped(me, bits_of(step), sp_count)
        return remote(SP, step, outgoing.at[peer], rows.at[step, 0], {"sp": peer})

    def across_copy(step):
        return remote(ACROSS, step, rows.at[step, 0], rows.at[step, 1], {"tp": across})

    def near_copy(step):
        return remote(NEAR, step, rows.at[step, 0], rows.at[step, 2], {"tp": mate})

    def near2_copy(step):
        return remote(NEAR2, step, rows.at[step, 1], rows.at[step, 3], {"tp": mate})

    def core_copy(step):
        return remote(CORE, step, part.at[step, pl.ds(2, 2)], core_in.at[step], {"tp": mate})

    def back_copy(step):
        return remote(BACK, step, y_out.at[step], y_in.at[step], {"tp": across})

    def home_copy(step):
        peer = flipped(me, bits_of(step), sp_count)
        return remote(HOME, step, done_out.at[step], returned.at[me], {"sp": peer})

    weights = [
        pltpu.make_async_copy(source, target, weight_sem.at[n])
        for n, (source, target) in enumerate(((gate_hbm, gate), (up_hbm, up), (down_hbm, down)))
    ]
    own_in = pltpu.make_async_copy(outgoing.at[me], rows.at[0, 0], local_sem.at[0])
    own_out = pltpu.make_async_copy(done_out.at[0], returned.at[me], local_sem.at[1])

    barrier = pltpu.get_barrier_semaphore()
    own_in.start()

    def greet(step, carry):
        pl.semaphore_signal(
            barrier, inc=1, device_id={"sp": flipped(me, step, sp_count)},
            device_id_type=pl.DeviceIdType.MESH,
        )
        return carry

    lax.fori_loop(1, sp_count, greet, 0)
    for near in (mate, across):
        pl.semaphore_signal(
            barrier, inc=1, device_id={"tp": near}, device_id_type=pl.DeviceIdType.MESH
        )
    pl.semaphore_wait(barrier, sp_count + 1)

    def send_out(step, carry):
        out_copy(step).start()
        return carry

    lax.fori_loop(1, sp_count, send_out, 0)
    for copy in weights:
        copy.start()
    own_in.wait()

    local_experts, width, units = gate.shape
    slots = rows.shape[2]
    chunk = tp_count * slots

    def forward(step):
        @pl.when(step > 0)
        def _():
            out_copy(step).wait_recv()

        across_copy(step).start()
        near_copy(step).start()

    def forward_again(step):
        across_copy(step).wait_recv()
        near2_copy(step).start()

    def compute(step):
        @pl.when(step == 0)
        def _():
            for copy in weights:
                copy.wait()

        near_copy(step).wait_recv()
        near2_copy(step).wait_recv()
        block = rows[step].reshape(chunk, width)
        hiddens = []
        for expert in range(local_experts):
            gate_pre = jnp.dot(block, gate[expert], preferred_element_type=jnp.float32)
            up_pre = jnp.dot(block, up[expert], preferred_element_type=jnp.float32)
            gated = jnp.minimum(gate_pre, 7.0)
            upper = jnp.clip(up_pre, -7.0, 7.0)
            hidden = (upper + 1.0) * gated * jax.nn.sigmoid(1.702 * gated)
            if local_experts > 1:
                row = lax.broadcasted_iota(jnp.int32, (chunk, units), 0)
                hidden = jnp.where((row // capacity) % local_experts == expert, hidden, 0.0)
            hiddens.append(hidden.astype(jnp.bfloat16))
        tile = width // 4
        for start in range(0, width, tile):
            total = jnp.dot(
                hiddens[0], down[0, :, start : start + tile], preferred_element_type=jnp.float32
            )
            for expert in range(1, local_experts):
                total = total + jnp.dot(
                    hiddens[expert], down[expert, :, start : start + tile],
                    preferred_element_type=jnp.float32,
                )
            part[step, :, :, start : start + tile] = total.astype(jnp.bfloat16).reshape(
                tp_count, slots, tile
            )
        core_copy(step).start()

    def add_core(step):
        core_copy(step).wait_recv()
        y_out[step] = (
            part[step, 1].astype(jnp.float32) + core_in[step, 1].astype(jnp.float32)
        ).astype(jnp.bfloat16)
        back_copy(step).start()

    def add_across(step):
        back_copy(step).wait_recv()
        done_out[step] = (
            part[step, 0].astype(jnp.float32)
            + core_in[step, 0].astype(jnp.float32)
            + y_in[step].astype(jnp.float32)
        ).astype(jnp.bfloat16)

        @pl.when(step == 0)
        def _():
            own_out.start()

        @pl.when(step > 0)
        def _():
            home_copy(step).start()

    stages = ((forward, 0), (forward_again, 1), (compute, 2), (add_core, 3), (add_across, 4))

    def turn(number, carry):
        for stage, lag in stages:
            step = number - lag

            @pl.when((step >= 0) & (step < sp_count))
            def _():
                stage(step)

        return carry

    lax.fori_loop(0, sp_count + 4, turn, 0)

    def finish(step, carry):
        @pl.when(step > 0)
        def _():
            out_copy(step).wait_send()
            home_copy(step).wait_send()
            home_copy(step).wait_recv()

        for make in (across_copy, near_copy, near2_copy, core_copy, back_copy):
            make(step).wait_send()
        return carry

    lax.fori_loop(0, sp_count, finish, 0)
    own_out.wait()


def run_experts(outgoing, gate_weight, up_weight, down_weight, capacity):
    sp_count, slots, width = outgoing.shape
    tp_count = lax.axis_size("tp")
    assert tp_count == 4
    local_experts, _, units = gate_weight.shape
    rows = sp_count * tp_count * slots
    half = jnp.bfloat16
    anywhere = pl.BlockSpec(memory_space=pl.ANY)
    return pl.pallas_call(
        functools.partial(expert_kernel, sp_count, tp_count, capacity),
        out_shape=jax.ShapeDtypeStruct(outgoing.shape, half),
        in_specs=[anywhere] * 4,
        out_specs=anywhere,
        scratch_shapes=[
            pltpu.VMEM(gate_weight.shape, half),
            pltpu.VMEM(up_weight.shape, half),
            pltpu.VMEM(down_weight.shape, half),
            pltpu.VMEM((sp_count, tp_count, slots, width), half),
            pltpu.VMEM((sp_count, tp_count, slots, width), half),
            pltpu.VMEM((sp_count, 2, slots, width), half),
            pltpu.VMEM((sp_count, slots, width), half),
            pltpu.VMEM((sp_count, slots, width), half),
            pltpu.VMEM((sp_count, slots, width), half),
            pltpu.SemaphoreType.DMA((3,)),
            pltpu.SemaphoreType.DMA((2,)),
            pltpu.SemaphoreType.DMA((7, sp_count)),
            pltpu.SemaphoreType.DMA((7, sp_count)),
        ],
        compiler_params=pltpu.CompilerParams(
            collective_id=0, has_side_effects=True, vmem_limit_bytes=60 * 1024 * 1024
        ),
        cost_estimate=pl.CostEstimate(
            flops=6 * rows * local_experts * width * units,
            bytes_accessed=6 * local_experts * width * units,
            transcendentals=rows * units,
        ),
        name="experts",
    )(outgoing, gate_weight, up_weight, down_weight)


def body(
    residual,
    queries,
    keys,
    values,
    documents,
    sink,
    out_weight,
    mix_gain,
    ffn_gain,
    out_gain,
    routes,
    route_logits,
    gate_weight,
    up_weight,
    down_weight,
):
    sp_count = lax.axis_size("sp")
    own_rows = residual.shape[0]
    all_heads = run_attention(queries, keys, values, documents, sink)
    projected = jnp.dot(all_heads, out_weight, preferred_element_type=jnp.float32)
    after_mix = residual.astype(jnp.float32) + rms_scale(projected) * mix_gain
    normed = (rms_scale(after_mix) * ffn_gain).astype(jnp.bfloat16)
    local_experts = gate_weight.shape[0]
    expert_count = local_experts * sp_count
    capacity = max(2, own_rows * TOPK * 4 // (3 * expert_count))
    exp_logits = jnp.exp(route_logits)
    route_weights = exp_logits / jnp.sum(exp_logits, axis=-1, keepdims=True)
    named = routes[:, :, None] == jnp.arange(expert_count, dtype=jnp.int32)
    hits = jnp.any(named, axis=1)
    expert_weights = jnp.sum(jnp.where(named, route_weights[:, :, None], 0.0), axis=1)
    row_ids = jnp.arange(own_rows, dtype=jnp.int32)
    lower = (row_ids[:, None] >= row_ids[None, :]).astype(jnp.bfloat16)
    places = jnp.dot(lower, hits.astype(jnp.bfloat16), preferred_element_type=jnp.float32)
    places = jnp.where(hits, places.astype(jnp.int32) - 1, -1)
    slot_ids = jnp.arange(capacity, dtype=jnp.int32)
    total_slots = expert_count * capacity
    chosen = places[:, :, None] == slot_ids
    pick = (places.T[:, None, :] == slot_ids[None, :, None]).reshape(total_slots, own_rows)
    outgoing = jnp.dot(
        pick.astype(jnp.bfloat16), normed, preferred_element_type=jnp.float32
    ).astype(jnp.bfloat16)
    model_width = normed.shape[1]
    outgoing = outgoing.reshape(sp_count, local_experts * capacity, model_width)
    returned = run_experts(outgoing, gate_weight, up_weight, down_weight, capacity)
    returned = returned.reshape(total_slots, model_width)
    high = expert_weights.astype(jnp.bfloat16).astype(jnp.float32)
    low = expert_weights - high

    def spread(weights):
        wide = jnp.where(chosen, weights[:, :, None], 0.0)
        return wide.reshape(own_rows, total_slots).astype(jnp.bfloat16)

    expert_mix = jnp.dot(spread(high), returned, preferred_element_type=jnp.float32)
    expert_mix = expert_mix + jnp.dot(spread(low), returned, preferred_element_type=jnp.float32)
    return (after_mix + rms_scale(expert_mix) * out_gain).astype(jnp.bfloat16)


def solution(mesh):
    in_specs = (
        P(("sp", "tp"), None),
        P("sp", "tp"),
        P("sp", "tp"),
        P("sp", "tp"),
        P("sp"),
        P("tp"),
        P(),
        P(),
        P(),
        P(),
        P(("sp", "tp"), None),
        P(("sp", "tp"), None),
        P("sp", None, "tp"),
        P("sp", None, "tp"),
        P("sp", "tp", None),
    )
    out_specs = P(("sp", "tp"), None)
    return jax.shard_map(body, mesh=mesh, in_specs=in_specs, out_specs=out_specs, check_vma=False)
```

```python
import functools

import jax
import jax.numpy as jnp
from jax import lax
from jax.experimental import pallas as pl
from jax.experimental.pallas import tpu as pltpu
from jax.sharding import PartitionSpec as P

HD = 64
TOPK = 4
W = 128
PIECES = 2


def rms_scale(vector):
    return vector * lax.rsqrt(jnp.mean(vector * vector, axis=-1, keepdims=True) + 1e-06)


def attention_kernel(
    sp_count, tp_count,
    queries, keys, values, documents, doc_column, cosine, sine, sink_terms,
    heads_out,
    wide_keys, wide_values, wide_docs, turned_keys, attended,
    local_sem, send_sem, recv_sem, out_send, out_recv,
):
    me = lax.axis_index("sp")
    tp = lax.axis_index("tp")
    right = (me + 1) % sp_count
    left = (me + sp_count - 1) % sp_count
    tok_rows, width = queries.shape
    blocks = tok_rows // W
    kv_count = keys.shape[1] // HD
    group_size = width // HD // kv_count
    own_rows = tok_rows // tp_count
    total = tok_rows * sp_count
    mesh_id = pl.DeviceIdType.MESH

    inside = pl.ds(W, tok_rows)
    locals_in = [
        pltpu.make_async_copy(source, target, local_sem.at[n])
        for n, (source, target) in enumerate(
            (
                (keys, wide_keys.at[inside]),
                (values, wide_values.at[inside]),
                (documents, wide_docs.at[pl.ds(1, blocks)]),
            )
        )
    ]
    for copy in locals_in:
        copy.start()

    barrier = pltpu.get_barrier_semaphore()
    for neighbour in (left, right):
        pl.semaphore_signal(barrier, inc=1, device_id={"sp": neighbour}, device_id_type=mesh_id)
    for hop in range(1, tp_count):
        pl.semaphore_signal(
            barrier, inc=1, device_id={"tp": (tp + hop) % tp_count}, device_id_type=mesh_id
        )
    pl.semaphore_wait(barrier, 2 + tp_count - 1)

    low, high = pl.ds(0, W), pl.ds(tok_rows + W, W)
    last = pl.ds(tok_rows - W, W)
    pairs = (
        (keys.at[last], wide_keys.at[low], right),
        (values.at[last], wide_values.at[low], right),
        (documents.at[blocks - 1], wide_docs.at[0], right),
        (keys.at[low], wide_keys.at[high], left),
        (values.at[low], wide_values.at[high], left),
        (documents.at[0], wide_docs.at[blocks + 1], left),
    )
    halos = [
        pltpu.make_async_remote_copy(
            src_ref=source, dst_ref=target, send_sem=send_sem.at[n], recv_sem=recv_sem.at[n],
            device_id={"sp": device}, device_id_type=mesh_id,
        )
        for n, (source, target, device) in enumerate(pairs)
    ]
    for copy in halos:
        copy.start()

    def turn(block, rows):
        size = block.shape[1]
        wide = block.astype(jnp.float32)
        lane = lax.broadcasted_iota(jnp.int32, block.shape, 1)
        swapped = jnp.where(
            lane % HD < HD // 2, jnp.roll(wide, -(HD // 2), 1), jnp.roll(wide, HD // 2, 1)
        )
        copies = size // HD
        cos = jnp.concatenate([cosine[rows, :]] * copies, axis=1)
        sin = jnp.concatenate([sine[rows, :]] * copies, axis=1)
        return (wide * cos + swapped * sin).astype(jnp.bfloat16)

    turned_queries = [
        turn(queries[n * W : (n + 1) * W, :], slice((n + 1) * W, (n + 2) * W))
        for n in range(blocks)
    ]
    for copy in locals_in:
        copy.wait()
    for copy in halos:
        copy.wait()
    for n in range(blocks + 2):
        rows = slice(n * W, (n + 1) * W)
        turned_keys[rows, :] = turn(wide_keys[rows, :], rows)

    scale = HD ** (-0.5)
    for n in range(blocks):
        start = me * tok_rows + n * W
        query_pos = lax.broadcasted_iota(jnp.int32, (W, 3 * W), 0) + W
        key_pos = lax.broadcasted_iota(jnp.int32, (W, 3 * W), 1)
        place = key_pos + (start - W)
        doc_keys = jnp.concatenate([wide_docs[n + m] for m in range(3)], axis=1)
        keep = (jnp.abs(query_pos - key_pos) <= W) & (place >= 0) & (place < total)
        keep = keep & (doc_column[n * W : (n + 1) * W, :] == doc_keys)
        for head in range(kv_count * group_size):
            kv = slice(head // group_size * HD, (head // group_size + 1) * HD)
            columns = slice(head * HD, (head + 1) * HD)
            window = slice(n * W, (n + 3) * W)
            scores = lax.dot_general(
                turned_queries[n][:, columns], turned_keys[window, kv],
                (((1,), (1,)), ((), ())), preferred_element_type=jnp.float32,
            ) * scale
            exponent = jnp.where(keep, jnp.exp(scores), 0.0)
            denominator = jnp.sum(exponent, axis=-1, keepdims=True) + sink_terms[head]
            probs = (exponent / denominator).astype(jnp.bfloat16)
            found = jnp.dot(probs, wide_values[window, kv], preferred_element_type=jnp.float32)
            attended[n * W : (n + 1) * W, columns] = found.astype(jnp.bfloat16)

    def share(index):
        return attended.at[pl.ds(pl.multiple_of(index * own_rows, own_rows), own_rows)]

    mine = heads_out.at[:, pl.ds(pl.multiple_of(tp * width, width), width)]
    sends = []
    for hop in range(1, tp_count):
        peer = (tp + hop) % tp_count
        sends.append(
            pltpu.make_async_remote_copy(
                src_ref=share(peer), dst_ref=mine, send_sem=out_send.at[hop],
                recv_sem=out_recv.at[hop], device_id={"tp": peer}, device_id_type=mesh_id,
            )
        )
    for copy in sends:
        copy.start()
    own = pltpu.make_async_copy(share(tp), mine, local_sem.at[3])
    own.start()
    own.wait()
    for copy in sends:
        copy.wait()


def run_attention(queries, keys, values, documents, sink):
    sp_count = lax.axis_size("sp")
    tp_count = lax.axis_size("tp")
    tok_rows, width = queries.shape
    blocks = tok_rows // W
    half_size = HD // 2
    first = lax.axis_index("sp") * tok_rows - W
    positions = first + jnp.arange(tok_rows + 2 * W, dtype=jnp.int32)
    inverse = 10000.0 ** (-jnp.arange(half_size, dtype=jnp.float32) / half_size)
    angles = positions.astype(jnp.float32)[:, None] * inverse[None, :]
    cosine, sine = jnp.cos(angles), jnp.sin(angles)
    cosine = jnp.concatenate([cosine, cosine], axis=1)
    sine = jnp.concatenate([-sine, sine], axis=1)
    vmem = pl.BlockSpec(memory_space=pltpu.VMEM)
    anywhere = pl.BlockSpec(memory_space=pl.ANY)
    half = jnp.bfloat16
    wide = tok_rows + 2 * W
    return pl.pallas_call(
        functools.partial(attention_kernel, sp_count, tp_count),
        out_shape=jax.ShapeDtypeStruct((tok_rows // tp_count, width * tp_count), half),
        in_specs=[vmem, anywhere, anywhere, anywhere, vmem, vmem, vmem,
                  pl.BlockSpec(memory_space=pltpu.SMEM)],
        out_specs=vmem,
        scratch_shapes=[
            pltpu.VMEM((wide, keys.shape[1]), half),
            pltpu.VMEM((wide, keys.shape[1]), half),
            pltpu.VMEM((blocks + 2, 1, W), jnp.int32),
            pltpu.VMEM((wide, keys.shape[1]), half),
            pltpu.VMEM((tok_rows, width), half),
            pltpu.SemaphoreType.DMA((4,)),
            pltpu.SemaphoreType.DMA((6,)),
            pltpu.SemaphoreType.DMA((6,)),
            pltpu.SemaphoreType.DMA((tp_count,)),
            pltpu.SemaphoreType.DMA((tp_count,)),
        ],
        compiler_params=pltpu.CompilerParams(collective_id=1, has_side_effects=True),
        cost_estimate=pl.CostEstimate(
            flops=4 * tok_rows * 3 * W * width,
            bytes_accessed=4 * tok_rows * width,
            transcendentals=tok_rows * 3 * W * width // HD,
        ),
        name="attention",
    )(
        queries, keys, values, documents.reshape(blocks, 1, W), documents[:, None],
        cosine, sine, jnp.exp(sink),
    )


def flipped(index, bits, size):
    result, unit = 0, 1
    while unit < size:
        result = result + ((index // unit + bits // unit) % 2) * unit
        unit *= 2
    return result


def expert_kernel(
    sp_count, tp_count, capacity,
    outgoing, gate_hbm, up_hbm, down_hbm,
    returned,
    gate, up, down, rows, part, core_in, y_out, y_in, done_out,
    weight_sem, local_sem, send_sem, recv_sem,
):
    me = lax.axis_index("sp")
    tp = lax.axis_index("tp")
    mate = flipped(tp, 1, tp_count)
    across = flipped(tp, 2, tp_count)
    SP, ACROSS, NEAR, NEAR2, CORE, BACK, HOME = range(7)

    pieces = outgoing.shape[1]
    steps = sp_count * pieces

    def bits_of(step):
        return step // pieces

    def remote(kind, step, source, target, device):
        return pltpu.make_async_remote_copy(
            src_ref=source,
            dst_ref=target,
            send_sem=send_sem.at[kind, step],
            recv_sem=recv_sem.at[kind, step],
            device_id=device,
            device_id_type=pl.DeviceIdType.MESH,
        )

    def out_copy(step):
        peer = flipped(me, bits_of(step), sp_count)
        return remote(SP, step, outgoing.at[peer, step % pieces], rows.at[step, 0], {"sp": peer})

    def across_copy(step):
        return remote(ACROSS, step, rows.at[step, 0], rows.at[step, 1], {"tp": across})

    def near_copy(step):
        return remote(NEAR, step, rows.at[step, 0], rows.at[step, 2], {"tp": mate})

    def near2_copy(step):
        return remote(NEAR2, step, rows.at[step, 1], rows.at[step, 3], {"tp": mate})

    def core_copy(step):
        return remote(CORE, step, part.at[step, pl.ds(2, 2)], core_in.at[step], {"tp": mate})

    def back_copy(step):
        return remote(BACK, step, y_out.at[step], y_in.at[step], {"tp": across})

    def home_copy(step):
        peer = flipped(me, bits_of(step), sp_count)
        return remote(HOME, step, done_out.at[step], returned.at[me, step % pieces], {"sp": peer})

    weights = [
        pltpu.make_async_copy(source, target, weight_sem.at[n])
        for n, (source, target) in enumerate(((gate_hbm, gate), (up_hbm, up), (down_hbm, down)))
    ]
    own_in = [
        pltpu.make_async_copy(outgoing.at[me, n], rows.at[n, 0], local_sem.at[0, n])
        for n in range(pieces)
    ]

    def own_out(step):
        return pltpu.make_async_copy(
            done_out.at[step], returned.at[me, step], local_sem.at[1, step]
        )

    barrier = pltpu.get_barrier_semaphore()
    for copy in own_in:
        copy.start()

    def greet(step, carry):
        pl.semaphore_signal(
            barrier, inc=1, device_id={"sp": flipped(me, step, sp_count)},
            device_id_type=pl.DeviceIdType.MESH,
        )
        return carry

    lax.fori_loop(1, sp_count, greet, 0)
    for near in (mate, across):
        pl.semaphore_signal(
            barrier, inc=1, device_id={"tp": near}, device_id_type=pl.DeviceIdType.MESH
        )
    pl.semaphore_wait(barrier, sp_count + 1)

    def send_out(step, carry):
        out_copy(step).start()
        return carry

    lax.fori_loop(pieces, steps, send_out, 0)
    for copy in weights:
        copy.start()
    for copy in own_in:
        copy.wait()

    local_experts, width, units = gate.shape
    slots = rows.shape[2]
    chunk = tp_count * slots

    def forward(step):
        @pl.when(step >= pieces)
        def _():
            out_copy(step).wait_recv()

        across_copy(step).start()
        near_copy(step).start()

    def forward_again(step):
        across_copy(step).wait_recv()
        near2_copy(step).start()

    def compute(step):
        @pl.when(step == 0)
        def _():
            for copy in weights:
                copy.wait()

        near_copy(step).wait_recv()
        near2_copy(step).wait_recv()
        block = rows[step].reshape(chunk, width)
        hiddens = []
        for expert in range(local_experts):
            gate_pre = jnp.dot(block, gate[expert], preferred_element_type=jnp.float32)
            up_pre = jnp.dot(block, up[expert], preferred_element_type=jnp.float32)
            gated = jnp.minimum(gate_pre, 7.0)
            upper = jnp.clip(up_pre, -7.0, 7.0)
            hidden = (upper + 1.0) * gated * jax.nn.sigmoid(1.702 * gated)
            if local_experts > 1:
                row = lax.broadcasted_iota(jnp.int32, (chunk, units), 0)
                slot = (step % pieces) * slots + row % slots
                hidden = jnp.where(slot // capacity == expert, hidden, 0.0)
            hiddens.append(hidden.astype(jnp.bfloat16))
        tile = width // 4
        for start in range(0, width, tile):
            total = jnp.dot(
                hiddens[0], down[0, :, start : start + tile], preferred_element_type=jnp.float32
            )
            for expert in range(1, local_experts):
                total = total + jnp.dot(
                    hiddens[expert], down[expert, :, start : start + tile],
                    preferred_element_type=jnp.float32,
                )
            part[step, :, :, start : start + tile] = total.astype(jnp.bfloat16).reshape(
                tp_count, slots, tile
            )
        core_copy(step).start()

    def add_core(step):
        core_copy(step).wait_recv()
        y_out[step] = (
            part[step, 1].astype(jnp.float32) + core_in[step, 1].astype(jnp.float32)
        ).astype(jnp.bfloat16)
        back_copy(step).start()

    def add_across(step):
        back_copy(step).wait_recv()
        done_out[step] = (
            part[step, 0].astype(jnp.float32)
            + core_in[step, 0].astype(jnp.float32)
            + y_in[step].astype(jnp.float32)
        ).astype(jnp.bfloat16)

        @pl.when(step < pieces)
        def _():
            own_out(step).start()

        @pl.when(step >= pieces)
        def _():
            home_copy(step).start()

    stages = ((forward, 0), (forward_again, 1), (compute, 2), (add_core, 3), (add_across, 4))

    def turn(number, carry):
        for stage, lag in stages:
            step = number - lag

            @pl.when((step >= 0) & (step < steps))
            def _():
                stage(step)

        return carry

    lax.fori_loop(0, steps + 4, turn, 0)

    def finish(step, carry):
        @pl.when(step >= pieces)
        def _():
            out_copy(step).wait_send()
            home_copy(step).wait_send()
            home_copy(step).wait_recv()

        for make in (across_copy, near_copy, near2_copy, core_copy, back_copy):
            make(step).wait_send()
        return carry

    lax.fori_loop(0, steps, finish, 0)
    for n in range(pieces):
        own_out(n).wait()


def run_experts(outgoing, gate_weight, up_weight, down_weight, capacity):
    sp_count, slots, width = outgoing.shape
    pieces = PIECES if slots % (16 * PIECES) == 0 else 1
    outgoing = outgoing.reshape(sp_count, pieces, slots // pieces, width)
    steps, slots = sp_count * pieces, slots // pieces
    tp_count = lax.axis_size("tp")
    assert tp_count == 4
    local_experts, _, units = gate_weight.shape
    rows = steps * tp_count * slots
    half = jnp.bfloat16
    anywhere = pl.BlockSpec(memory_space=pl.ANY)
    return pl.pallas_call(
        functools.partial(expert_kernel, sp_count, tp_count, capacity),
        out_shape=jax.ShapeDtypeStruct(outgoing.shape, half),
        in_specs=[anywhere] * 4,
        out_specs=anywhere,
        scratch_shapes=[
            pltpu.VMEM(gate_weight.shape, half),
            pltpu.VMEM(up_weight.shape, half),
            pltpu.VMEM(down_weight.shape, half),
            pltpu.VMEM((steps, tp_count, slots, width), half),
            pltpu.VMEM((steps, tp_count, slots, width), half),
            pltpu.VMEM((steps, 2, slots, width), half),
            pltpu.VMEM((steps, slots, width), half),
            pltpu.VMEM((steps, slots, width), half),
            pltpu.VMEM((steps, slots, width), half),
            pltpu.SemaphoreType.DMA((3,)),
            pltpu.SemaphoreType.DMA((2, pieces)),
            pltpu.SemaphoreType.DMA((7, steps)),
            pltpu.SemaphoreType.DMA((7, steps)),
        ],
        compiler_params=pltpu.CompilerParams(
            collective_id=0, has_side_effects=True, vmem_limit_bytes=60 * 1024 * 1024
        ),
        cost_estimate=pl.CostEstimate(
            flops=6 * rows * local_experts * width * units,
            bytes_accessed=6 * local_experts * width * units,
            transcendentals=rows * units,
        ),
        name="experts",
    )(outgoing, gate_weight, up_weight, down_weight)


def body(
    residual,
    queries,
    keys,
    values,
    documents,
    sink,
    out_weight,
    mix_gain,
    ffn_gain,
    out_gain,
    routes,
    route_logits,
    gate_weight,
    up_weight,
    down_weight,
):
    sp_count = lax.axis_size("sp")
    own_rows = residual.shape[0]
    all_heads = run_attention(queries, keys, values, documents, sink)
    projected = jnp.dot(all_heads, out_weight, preferred_element_type=jnp.float32)
    after_mix = residual.astype(jnp.float32) + rms_scale(projected) * mix_gain
    normed = (rms_scale(after_mix) * ffn_gain).astype(jnp.bfloat16)
    local_experts = gate_weight.shape[0]
    expert_count = local_experts * sp_count
    capacity = max(2, own_rows * TOPK * 4 // (3 * expert_count))
    exp_logits = jnp.exp(route_logits)
    route_weights = exp_logits / jnp.sum(exp_logits, axis=-1, keepdims=True)
    named = routes[:, :, None] == jnp.arange(expert_count, dtype=jnp.int32)
    hits = jnp.any(named, axis=1)
    expert_weights = jnp.sum(jnp.where(named, route_weights[:, :, None], 0.0), axis=1)
    row_ids = jnp.arange(own_rows, dtype=jnp.int32)
    lower = (row_ids[:, None] >= row_ids[None, :]).astype(jnp.bfloat16)
    places = jnp.dot(lower, hits.astype(jnp.bfloat16), preferred_element_type=jnp.float32)
    places = jnp.where(hits, places.astype(jnp.int32) - 1, -1)
    slot_ids = jnp.arange(capacity, dtype=jnp.int32)
    total_slots = expert_count * capacity
    chosen = places[:, :, None] == slot_ids
    pick = (places.T[:, None, :] == slot_ids[None, :, None]).reshape(total_slots, own_rows)
    outgoing = jnp.dot(
        pick.astype(jnp.bfloat16), normed, preferred_element_type=jnp.float32
    ).astype(jnp.bfloat16)
    model_width = normed.shape[1]
    outgoing = outgoing.reshape(sp_count, local_experts * capacity, model_width)
    returned = run_experts(outgoing, gate_weight, up_weight, down_weight, capacity)
    returned = returned.reshape(total_slots, model_width)
    high = expert_weights.astype(jnp.bfloat16).astype(jnp.float32)
    low = expert_weights - high

    def spread(weights):
        wide = jnp.where(chosen, weights[:, :, None], 0.0)
        return wide.reshape(own_rows, total_slots).astype(jnp.bfloat16)

    expert_mix = jnp.dot(spread(high), returned, preferred_element_type=jnp.float32)
    expert_mix = expert_mix + jnp.dot(spread(low), returned, preferred_element_type=jnp.float32)
    return (after_mix + rms_scale(expert_mix) * out_gain).astype(jnp.bfloat16)


def solution(mesh):
    in_specs = (
        P(("sp", "tp"), None),
        P("sp", "tp"),
        P("sp", "tp"),
        P("sp", "tp"),
        P("sp"),
        P("tp"),
        P(),
        P(),
        P(),
        P(),
        P(("sp", "tp"), None),
        P(("sp", "tp"), None),
        P("sp", None, "tp"),
        P("sp", None, "tp"),
        P("sp", "tp", None),
    )
    out_specs = P(("sp", "tp"), None)
    return jax.shard_map(body, mesh=mesh, in_specs=in_specs, out_specs=out_specs, check_vma=False)
```

```python
import functools

import jax
import jax.numpy as jnp
from jax import lax
from jax.experimental import pallas as pl
from jax.experimental.pallas import tpu as pltpu
from jax.sharding import PartitionSpec as P

HD = 64
TOPK = 4
W = 128
PIECES = 2


def rms_scale(vector):
    return vector * lax.rsqrt(jnp.mean(vector * vector, axis=-1, keepdims=True) + 1e-06)


def attention_kernel(
    sp_count, tp_count,
    queries, paired, documents, doc_column, cosine, sine, sink_logits,
    heads_out,
    wide_pairs, wide_docs, turned_keys, attended,
    local_sem, send_sem, recv_sem, out_send, out_recv,
):
    me = lax.axis_index("sp")
    tp = lax.axis_index("tp")
    right = (me + 1) % sp_count
    left = (me + sp_count - 1) % sp_count
    tok_rows, width = queries.shape
    blocks = tok_rows // W
    kv_width = paired.shape[1] // 2
    kv_count = kv_width // HD
    group_size = width // HD // kv_count
    own_rows = tok_rows // tp_count
    total = tok_rows * sp_count
    mesh_id = pl.DeviceIdType.MESH

    inside = pl.ds(W, tok_rows)
    locals_in = [
        pltpu.make_async_copy(source, target, local_sem.at[n])
        for n, (source, target) in enumerate(
            (
                (paired, wide_pairs.at[inside]),
                (documents, wide_docs.at[pl.ds(1, blocks)]),
            )
        )
    ]
    for copy in locals_in:
        copy.start()

    barrier = pltpu.get_barrier_semaphore()
    for neighbour in (left, right):
        pl.semaphore_signal(barrier, inc=1, device_id={"sp": neighbour}, device_id_type=mesh_id)
    for hop in range(1, tp_count):
        pl.semaphore_signal(
            barrier, inc=1, device_id={"tp": (tp + hop) % tp_count}, device_id_type=mesh_id
        )
    pl.semaphore_wait(barrier, 2 + tp_count - 1)

    low, high = pl.ds(0, W), pl.ds(tok_rows + W, W)
    last = pl.ds(tok_rows - W, W)
    pairs = (
        (paired.at[last], wide_pairs.at[low], right),
        (documents.at[blocks - 1], wide_docs.at[0], right),
        (paired.at[low], wide_pairs.at[high], left),
        (documents.at[0], wide_docs.at[blocks + 1], left),
    )
    halos = [
        pltpu.make_async_remote_copy(
            src_ref=source, dst_ref=target, send_sem=send_sem.at[n], recv_sem=recv_sem.at[n],
            device_id={"sp": device}, device_id_type=mesh_id,
        )
        for n, (source, target, device) in enumerate(pairs)
    ]
    for copy in halos:
        copy.start()

    def turn(block, rows):
        size = block.shape[1]
        wide = block.astype(jnp.float32)
        lane = lax.broadcasted_iota(jnp.int32, block.shape, 1)
        swapped = jnp.where(
            lane % HD < HD // 2, jnp.roll(wide, -(HD // 2), 1), jnp.roll(wide, HD // 2, 1)
        )
        copies = size // HD
        cos = jnp.concatenate([cosine[rows, :]] * copies, axis=1)
        sin = jnp.concatenate([sine[rows, :]] * copies, axis=1)
        return (wide * cos + swapped * sin).astype(jnp.bfloat16)

    turned_queries = [
        turn(queries[n * W : (n + 1) * W, :], slice((n + 1) * W, (n + 2) * W))
        for n in range(blocks)
    ]
    for copy in locals_in:
        copy.wait()
    for copy in halos:
        copy.wait()
    for n in range(blocks + 2):
        rows = slice(n * W, (n + 1) * W)
        turned_keys[rows, :] = turn(wide_pairs[rows, :kv_width], rows)

    scale = HD ** (-0.5)
    for n in range(blocks):
        start = me * tok_rows + n * W
        query_pos = lax.broadcasted_iota(jnp.int32, (W, 3 * W), 0) + W
        key_pos = lax.broadcasted_iota(jnp.int32, (W, 3 * W), 1)
        place = key_pos + (start - W)
        doc_keys = jnp.concatenate([wide_docs[n + m] for m in range(3)], axis=1)
        keep = (jnp.abs(query_pos - key_pos) <= W) & (place >= 0) & (place < total)
        keep = keep & (doc_column[n * W : (n + 1) * W, :] == doc_keys)
        for head in range(kv_count * group_size):
            kv = slice(head // group_size * HD, (head // group_size + 1) * HD)
            columns = slice(head * HD, (head + 1) * HD)
            window = slice(n * W, (n + 3) * W)
            scores = lax.dot_general(
                turned_queries[n][:, columns], turned_keys[window, kv],
                (((1,), (1,)), ((), ())), preferred_element_type=jnp.float32,
            ) * scale
            exponent = jnp.where(keep, jnp.exp(scores), 0.0)
            sink_term = jnp.exp(jnp.full((W, 1), sink_logits[head], jnp.float32))
            denominator = jnp.sum(exponent, axis=-1, keepdims=True) + sink_term
            probs = (exponent / denominator).astype(jnp.bfloat16)
            held = slice(kv_width + kv.start, kv_width + kv.stop)
            found = jnp.dot(probs, wide_pairs[window, held], preferred_element_type=jnp.float32)
            attended[n * W : (n + 1) * W, columns] = found.astype(jnp.bfloat16)

    def share(index):
        return attended.at[pl.ds(pl.multiple_of(index * own_rows, own_rows), own_rows)]

    mine = heads_out.at[:, pl.ds(pl.multiple_of(tp * width, width), width)]
    sends = []
    for hop in range(1, tp_count):
        peer = (tp + hop) % tp_count
        sends.append(
            pltpu.make_async_remote_copy(
                src_ref=share(peer), dst_ref=mine, send_sem=out_send.at[hop],
                recv_sem=out_recv.at[hop], device_id={"tp": peer}, device_id_type=mesh_id,
            )
        )
    for copy in sends:
        copy.start()
    own = pltpu.make_async_copy(share(tp), mine, local_sem.at[3])
    own.start()
    own.wait()
    for copy in sends:
        copy.wait()


def run_attention(queries, keys, values, documents, sink):
    sp_count = lax.axis_size("sp")
    tp_count = lax.axis_size("tp")
    tok_rows, width = queries.shape
    blocks = tok_rows // W
    half_size = HD // 2
    first = lax.axis_index("sp") * tok_rows - W
    positions = first + jnp.arange(tok_rows + 2 * W, dtype=jnp.int32)
    inverse = 10000.0 ** (-jnp.arange(half_size, dtype=jnp.float32) / half_size)
    angles = positions.astype(jnp.float32)[:, None] * inverse[None, :]
    cosine, sine = jnp.cos(angles), jnp.sin(angles)
    cosine = jnp.concatenate([cosine, cosine], axis=1)
    sine = jnp.concatenate([-sine, sine], axis=1)
    vmem = pl.BlockSpec(memory_space=pltpu.VMEM)
    anywhere = pl.BlockSpec(memory_space=pl.ANY)
    half = jnp.bfloat16
    wide = tok_rows + 2 * W
    return pl.pallas_call(
        functools.partial(attention_kernel, sp_count, tp_count),
        out_shape=jax.ShapeDtypeStruct((tok_rows // tp_count, width * tp_count), half),
        in_specs=[vmem, anywhere, anywhere, vmem, vmem, vmem,
                  pl.BlockSpec(memory_space=pltpu.SMEM)],
        out_specs=vmem,
        scratch_shapes=[
            pltpu.VMEM((wide, 2 * keys.shape[1]), half),
            pltpu.VMEM((blocks + 2, 1, W), jnp.int32),
            pltpu.VMEM((wide, keys.shape[1]), half),
            pltpu.VMEM((tok_rows, width), half),
            pltpu.SemaphoreType.DMA((4,)),
            pltpu.SemaphoreType.DMA((4,)),
            pltpu.SemaphoreType.DMA((4,)),
            pltpu.SemaphoreType.DMA((tp_count,)),
            pltpu.SemaphoreType.DMA((tp_count,)),
        ],
        compiler_params=pltpu.CompilerParams(collective_id=1, has_side_effects=True),
        cost_estimate=pl.CostEstimate(
            flops=4 * tok_rows * 3 * W * width,
            bytes_accessed=4 * tok_rows * width,
            transcendentals=tok_rows * 3 * W * width // HD,
        ),
        name="attention",
    )(
        queries, jnp.concatenate([keys, values], axis=1), documents.reshape(blocks, 1, W),
        documents[:, None], cosine, sine, sink,
    )


def flipped(index, bits, size):
    result, unit = 0, 1
    while unit < size:
        result = result + ((index // unit + bits // unit) % 2) * unit
        unit *= 2
    return result


def expert_kernel(
    sp_count, tp_count, capacity,
    outgoing, gate_hbm, up_hbm, down_hbm,
    returned,
    gate, up, down, rows, part, core_in, y_out, y_in, done_out,
    weight_sem, local_sem, send_sem, recv_sem,
):
    me = lax.axis_index("sp")
    tp = lax.axis_index("tp")
    mate = flipped(tp, 1, tp_count)
    across = flipped(tp, 2, tp_count)
    SP, ACROSS, NEAR, NEAR2, CORE, BACK, HOME = range(7)

    pieces = outgoing.shape[1]
    steps = sp_count * pieces

    def bits_of(step):
        return step // pieces

    def remote(kind, step, source, target, device):
        return pltpu.make_async_remote_copy(
            src_ref=source,
            dst_ref=target,
            send_sem=send_sem.at[kind, step],
            recv_sem=recv_sem.at[kind, step],
            device_id=device,
            device_id_type=pl.DeviceIdType.MESH,
        )

    def out_copy(step):
        peer = flipped(me, bits_of(step), sp_count)
        return remote(SP, step, outgoing.at[peer, step % pieces], rows.at[step, 0], {"sp": peer})

    def across_copy(step):
        return remote(ACROSS, step, rows.at[step, 0], rows.at[step, 1], {"tp": across})

    def near_copy(step):
        return remote(NEAR, step, rows.at[step, 0], rows.at[step, 2], {"tp": mate})

    def near2_copy(step):
        return remote(NEAR2, step, rows.at[step, 1], rows.at[step, 3], {"tp": mate})

    def core_copy(step):
        return remote(CORE, step, part.at[step, pl.ds(2, 2)], core_in.at[step], {"tp": mate})

    def back_copy(step):
        return remote(BACK, step, y_out.at[step], y_in.at[step], {"tp": across})

    def home_copy(step):
        peer = flipped(me, bits_of(step), sp_count)
        return remote(HOME, step, done_out.at[step], returned.at[me, step % pieces], {"sp": peer})

    weights = [
        pltpu.make_async_copy(source, target, weight_sem.at[n])
        for n, (source, target) in enumerate(((gate_hbm, gate), (up_hbm, up), (down_hbm, down)))
    ]
    own_in = [
        pltpu.make_async_copy(outgoing.at[me, n], rows.at[n, 0], local_sem.at[0, n])
        for n in range(pieces)
    ]

    def own_out(step):
        return pltpu.make_async_copy(
            done_out.at[step], returned.at[me, step], local_sem.at[1, step]
        )

    barrier = pltpu.get_barrier_semaphore()
    for copy in own_in:
        copy.start()

    def greet(step, carry):
        pl.semaphore_signal(
            barrier, inc=1, device_id={"sp": flipped(me, step, sp_count)},
            device_id_type=pl.DeviceIdType.MESH,
        )
        return carry

    lax.fori_loop(1, sp_count, greet, 0)
    for near in (mate, across):
        pl.semaphore_signal(
            barrier, inc=1, device_id={"tp": near}, device_id_type=pl.DeviceIdType.MESH
        )
    pl.semaphore_wait(barrier, sp_count + 1)

    def send_out(step, carry):
        out_copy(step).start()
        return carry

    lax.fori_loop(pieces, steps, send_out, 0)
    for copy in weights:
        copy.start()
    for copy in own_in:
        copy.wait()

    local_experts, width, units = gate.shape
    slots = rows.shape[2]
    chunk = tp_count * slots

    def forward(step):
        @pl.when(step >= pieces)
        def _():
            out_copy(step).wait_recv()

        across_copy(step).start()
        near_copy(step).start()

    def forward_again(step):
        across_copy(step).wait_recv()
        near2_copy(step).start()

    def compute(step):
        @pl.when(step == 0)
        def _():
            for copy in weights:
                copy.wait()

        near_copy(step).wait_recv()
        near2_copy(step).wait_recv()
        block = rows[step].reshape(chunk, width)
        hiddens = []
        for expert in range(local_experts):
            gate_pre = jnp.dot(block, gate[expert], preferred_element_type=jnp.float32)
            up_pre = jnp.dot(block, up[expert], preferred_element_type=jnp.float32)
            gated = jnp.minimum(gate_pre, 7.0)
            upper = jnp.clip(up_pre, -7.0, 7.0)
            hidden = (upper + 1.0) * gated * jax.nn.sigmoid(1.702 * gated)
            if local_experts > 1:
                row = lax.broadcasted_iota(jnp.int32, (chunk, units), 0)
                slot = (step % pieces) * slots + row % slots
                hidden = jnp.where(slot // capacity == expert, hidden, 0.0)
            hiddens.append(hidden.astype(jnp.bfloat16))
        tile = width // 4
        for start in range(0, width, tile):
            total = jnp.dot(
                hiddens[0], down[0, :, start : start + tile], preferred_element_type=jnp.float32
            )
            for expert in range(1, local_experts):
                total = total + jnp.dot(
                    hiddens[expert], down[expert, :, start : start + tile],
                    preferred_element_type=jnp.float32,
                )
            part[step, :, :, start : start + tile] = total.astype(jnp.bfloat16).reshape(
                tp_count, slots, tile
            )
        core_copy(step).start()

    def add_core(step):
        core_copy(step).wait_recv()
        y_out[step] = (
            part[step, 1].astype(jnp.float32) + core_in[step, 1].astype(jnp.float32)
        ).astype(jnp.bfloat16)
        back_copy(step).start()

    def add_across(step):
        back_copy(step).wait_recv()
        done_out[step] = (
            part[step, 0].astype(jnp.float32)
            + core_in[step, 0].astype(jnp.float32)
            + y_in[step].astype(jnp.float32)
        ).astype(jnp.bfloat16)

        @pl.when(step < pieces)
        def _():
            own_out(step).start()

        @pl.when(step >= pieces)
        def _():
            home_copy(step).start()

    stages = ((forward, 0), (forward_again, 1), (add_core, 3), (add_across, 4), (compute, 2))

    def turn(number, carry):
        for stage, lag in stages:
            step = number - lag

            @pl.when((step >= 0) & (step < steps))
            def _():
                stage(step)

        return carry

    lax.fori_loop(0, steps + 4, turn, 0)

    def finish(step, carry):
        @pl.when(step >= pieces)
        def _():
            out_copy(step).wait_send()
            home_copy(step).wait_send()
            home_copy(step).wait_recv()

        for make in (across_copy, near_copy, near2_copy, core_copy, back_copy):
            make(step).wait_send()
        return carry

    lax.fori_loop(0, steps, finish, 0)
    for n in range(pieces):
        own_out(n).wait()


def run_experts(outgoing, gate_weight, up_weight, down_weight, capacity):
    sp_count, slots, width = outgoing.shape
    pieces = PIECES if slots % (16 * PIECES) == 0 else 1
    outgoing = outgoing.reshape(sp_count, pieces, slots // pieces, width)
    steps, slots = sp_count * pieces, slots // pieces
    tp_count = lax.axis_size("tp")
    assert tp_count == 4
    local_experts, _, units = gate_weight.shape
    rows = steps * tp_count * slots
    half = jnp.bfloat16
    anywhere = pl.BlockSpec(memory_space=pl.ANY)
    return pl.pallas_call(
        functools.partial(expert_kernel, sp_count, tp_count, capacity),
        out_shape=jax.ShapeDtypeStruct(outgoing.shape, half),
        in_specs=[anywhere] * 4,
        out_specs=anywhere,
        scratch_shapes=[
            pltpu.VMEM(gate_weight.shape, half),
            pltpu.VMEM(up_weight.shape, half),
            pltpu.VMEM(down_weight.shape, half),
            pltpu.VMEM((steps, tp_count, slots, width), half),
            pltpu.VMEM((steps, tp_count, slots, width), half),
            pltpu.VMEM((steps, 2, slots, width), half),
            pltpu.VMEM((steps, slots, width), half),
            pltpu.VMEM((steps, slots, width), half),
            pltpu.VMEM((steps, slots, width), half),
            pltpu.SemaphoreType.DMA((3,)),
            pltpu.SemaphoreType.DMA((2, pieces)),
            pltpu.SemaphoreType.DMA((7, steps)),
            pltpu.SemaphoreType.DMA((7, steps)),
        ],
        compiler_params=pltpu.CompilerParams(
            collective_id=0, has_side_effects=True, vmem_limit_bytes=60 * 1024 * 1024
        ),
        cost_estimate=pl.CostEstimate(
            flops=6 * rows * local_experts * width * units,
            bytes_accessed=6 * local_experts * width * units,
            transcendentals=rows * units,
        ),
        name="experts",
    )(outgoing, gate_weight, up_weight, down_weight)


def body(
    residual,
    queries,
    keys,
    values,
    documents,
    sink,
    out_weight,
    mix_gain,
    ffn_gain,
    out_gain,
    routes,
    route_logits,
    gate_weight,
    up_weight,
    down_weight,
):
    sp_count = lax.axis_size("sp")
    own_rows = residual.shape[0]
    all_heads = run_attention(queries, keys, values, documents, sink)
    projected = jnp.dot(all_heads, out_weight, preferred_element_type=jnp.float32)
    after_mix = residual.astype(jnp.float32) + rms_scale(projected) * mix_gain
    normed = (rms_scale(after_mix) * ffn_gain).astype(jnp.bfloat16)
    local_experts = gate_weight.shape[0]
    expert_count = local_experts * sp_count
    capacity = max(2, own_rows * TOPK * 4 // (3 * expert_count))
    exp_logits = jnp.exp(route_logits)
    route_weights = exp_logits / jnp.sum(exp_logits, axis=-1, keepdims=True)
    named = routes[:, :, None] == jnp.arange(expert_count, dtype=jnp.int32)
    hits = jnp.any(named, axis=1)
    expert_weights = jnp.sum(jnp.where(named, route_weights[:, :, None], 0.0), axis=1)
    row_ids = jnp.arange(own_rows, dtype=jnp.int32)
    lower = (row_ids[:, None] >= row_ids[None, :]).astype(jnp.bfloat16)
    places = jnp.dot(lower, hits.astype(jnp.bfloat16), preferred_element_type=jnp.float32)
    places = jnp.where(hits, places.astype(jnp.int32) - 1, -1)
    slot_ids = jnp.arange(capacity, dtype=jnp.int32)
    total_slots = expert_count * capacity
    chosen = places[:, :, None] == slot_ids
    pick = (places.T[:, None, :] == slot_ids[None, :, None]).reshape(total_slots, own_rows)
    outgoing = jnp.dot(
        pick.astype(jnp.bfloat16), normed, preferred_element_type=jnp.float32
    ).astype(jnp.bfloat16)
    model_width = normed.shape[1]
    outgoing = outgoing.reshape(sp_count, local_experts * capacity, model_width)
    returned = run_experts(outgoing, gate_weight, up_weight, down_weight, capacity)
    returned = returned.reshape(total_slots, model_width)
    high = expert_weights.astype(jnp.bfloat16).astype(jnp.float32)
    low = expert_weights - high

    def spread(weights):
        wide = jnp.where(chosen, weights[:, :, None], 0.0)
        return wide.reshape(own_rows, total_slots).astype(jnp.bfloat16)

    expert_mix = jnp.dot(spread(high), returned, preferred_element_type=jnp.float32)
    expert_mix = expert_mix + jnp.dot(spread(low), returned, preferred_element_type=jnp.float32)
    return (after_mix + rms_scale(expert_mix) * out_gain).astype(jnp.bfloat16)


def solution(mesh):
    in_specs = (
        P(("sp", "tp"), None),
        P("sp", "tp"),
        P("sp", "tp"),
        P("sp", "tp"),
        P("sp"),
        P("tp"),
        P(),
        P(),
        P(),
        P(),
        P(("sp", "tp"), None),
        P(("sp", "tp"), None),
        P("sp", None, "tp"),
        P("sp", None, "tp"),
        P("sp", "tp", None),
    )
    out_specs = P(("sp", "tp"), None)
    return jax.shard_map(body, mesh=mesh, in_specs=in_specs, out_specs=out_specs, check_vma=False)
```
